32 devices in a mesh: sp: 8 (over z, y), tp: 4 (over x, core).
Axes of the slice: x: 2, y: 2, z: 4, core: 2. Of those that a mesh axis runs over, the one named last changes fastest.
Arguments:
- stream_in: bfloat16 [6144, 2048], P(('sp', 'tp')), may hold values from -6 to 6
- query_wide: bfloat16 [6144, 512], P('sp', 'tp'), may hold values from -6 to 6
- key_wide: bfloat16 [6144, 512], P('sp', 'tp'), may hold values from -6 to 6
- value_wide: bfloat16 [6144, 512], P('sp', 'tp'), may hold values from -6 to 6
- gate_wide: bfloat16 [6144, 512], P('sp', 'tp'), may hold values from -6 to 6
- decay_wide: float32 [4, 6144], P('tp', 'sp'), may hold values from -2.3 to 0, as said below
- query_narrow: bfloat16 [6144, 512], P('sp', 'tp'), may hold values from -6 to 6
- key_narrow: bfloat16 [6144, 512], P('sp', 'tp'), may hold values from -6 to 6
- value_narrow: bfloat16 [6144, 512], P('sp', 'tp'), may hold values from -6 to 6
- gate_narrow: bfloat16 [6144, 512], P('sp', 'tp'), may hold values from -6 to 6
- decay_narrow: float32 [8, 6144], P('tp', 'sp'), may hold values from -2.3 to 0, as said below
- output_wide: bfloat16 [512, 2048], P('tp'), may hold values from -0.25 to 0.25
- output_narrow: bfloat16 [512, 2048], P('tp'), may hold values from -0.25 to 0.25
- norm_gain: bfloat16 [2048], replicated, may hold values from 0.099609375 to 1.8984375
- up_weight: bfloat16 [2048, 8192], P('sp', 'tp'), may hold values from -0.125 to 0.125
- down_weight: bfloat16 [8192, 2048], P('tp', 'sp'), may hold values from -0.0625 to 0.0625
Outputs:
- layer_out: bfloat16 [6144, 2048], P(('sp', 'tp'))
The draws below stay inside these ranges and needn't reach their ends.
Inputs may be any that keep to these rules, and one draw needn't show every extreme that they name: `decay_wide`: each entry is the logarithm of one head's retention factor at one position. `decay_narrow`: each entry is the logarithm of one head's retention factor at one position.
All inputs are finite; a program needn't handle non-finite values.
Results may differ from the reference program's by a relative error of at most 0.02.
Values may be sent and summed in bfloat16 or wider, within the bound.
A program may use at most 128 MiB of HBM per device.

```python
import math
import jax
import jax.numpy as jnp
from jax import lax

D = 2048
FF = 8192
HEADS_W = 4
HEADS_N = 8
HDW = 128
HDN = 64
BLOCK = 128
TOK_DEV = 768
RW = 512
RN = 512
TOKEN_POSITIONS = 6144


spike_count = 3


def log_decay_table(key, count_of_heads, slow_share):
    random_subkey_list = jax.random.split(key, 6)
    slow_heads = jax.random.uniform(random_subkey_list[0], (count_of_heads,), jnp.float32) < slow_share
    slow_rate = jax.random.uniform(random_subkey_list[1], (count_of_heads,), jnp.float32, 0.15, 0.4) * math.log(10.0) / TOKEN_POSITIONS
    fast_rate = 1.0 / jax.random.uniform(random_subkey_list[2], (count_of_heads,), jnp.float32, 30.0, 100.0)
    decay_rate = jnp.where(slow_heads, slow_rate, fast_rate)
    stretch = jnp.exp(jax.random.uniform(random_subkey_list[3], (TOKEN_POSITIONS // TOK_DEV,), jnp.float32, -math.log(2.0), math.log(2.0)))
    stretch = jnp.repeat(stretch, TOK_DEV)
    logarithm_base = -decay_rate[:, None] * stretch[None, :]
    spike_locations = jax.random.randint(random_subkey_list[4], (spike_count,), 0, TOKEN_POSITIONS)
    spike_labels = (jnp.arange(TOKEN_POSITIONS)[None, :] == spike_locations[:, None]).astype(jnp.float32)
    spike_removals = jax.random.uniform(random_subkey_list[5], (count_of_heads, spike_count), jnp.float32, math.log(0.5), math.log(0.8))
    return logarithm_base + jnp.dot(spike_removals, spike_labels)


def draw_decay_wide(key, part):
    share = 0.5
    return log_decay_table(jax.random.fold_in(key, 11), HEADS_W, share)


def draw_decay_narrow(key, part):
    share = 0.5
    return log_decay_table(jax.random.fold_in(key, 23), HEADS_N, share)


def steps_of(own_key, extent, shards, least, largest):
    def one(position, blocks):
        draws = jax.random.uniform(jax.random.fold_in(jax.random.fold_in(own_key, 6), position), (blocks,), jnp.float32, least / len(shards), largest / len(shards))
        return jnp.repeat(jnp.exp(draws), extent[position] // blocks).reshape((-1,) + (1,) * (len(extent) - position - 1))

    level = one(*shards[0])
    for cut in shards[1:]:
        level = level * one(*cut)
    return level


def scatter_about(key, extent, scale, most, pieces=(), kind=jnp.bfloat16):
    loudness = steps_of(key, extent, pieces, -0.22, 0.18) if pieces else 1.0
    drawn = jax.random.normal(key, extent, jnp.float32) * scale * loudness
    return jnp.minimum(jnp.maximum(drawn, -most), most).astype(kind)


def setup_inputs(seed: int = 0) -> dict:
    splits = jax.random.split(jax.random.key(seed), 17)
    return {
        "stream_in": scatter_about(splits[0], (TOKEN_POSITIONS, D), 1.0, 6.0, ((0, 32),)),
        "query_wide": scatter_about(splits[1], (TOKEN_POSITIONS, RW), 1.0, 6.0, ((0, 8), (1, 4))),
        "key_wide": scatter_about(splits[2], (TOKEN_POSITIONS, RW), 1.0, 6.0, ((0, 8), (1, 4))),
        "value_wide": scatter_about(splits[3], (TOKEN_POSITIONS, RW), 1.0, 6.0, ((0, 8), (1, 4))),
        "gate_wide": scatter_about(splits[4], (TOKEN_POSITIONS, RW), 1.0, 6.0, ((0, 8), (1, 4))),
        "decay_wide": draw_decay_wide(jax.random.fold_in(splits[16], 71), 0),
        "query_narrow": scatter_about(splits[6], (TOKEN_POSITIONS, RN), 1.0, 6.0, ((0, 8), (1, 4))),
        "key_narrow": scatter_about(splits[7], (TOKEN_POSITIONS, RN), 1.0, 6.0, ((0, 8), (1, 4))),
        "value_narrow": scatter_about(splits[8], (TOKEN_POSITIONS, RN), 1.0, 6.0, ((0, 8), (1, 4))),
        "gate_narrow": scatter_about(splits[9], (TOKEN_POSITIONS, RN), 1.0, 6.0, ((0, 8), (1, 4))),
        "decay_narrow": draw_decay_narrow(jax.random.fold_in(splits[16], 71), 0),
        "output_wide": scatter_about(splits[11], (RW, D), RW ** -0.5, 0.25, ((0, 4),)),
        "output_narrow": scatter_about(splits[12], (RN, D), RN ** -0.5, 0.25, ((0, 4),)),
        "norm_gain": jnp.clip(1.0 + 0.18 * jax.random.normal(splits[13], (D,), jnp.float32), 0.099609375, 1.8984375).astype(jnp.bfloat16),
        "up_weight": scatter_about(splits[14], (D, FF), D ** -0.5, 0.125, ((0, 8), (1, 4))),
        "down_weight": scatter_about(splits[15], (FF, D), FF ** -0.5, 0.0625, ((0, 4), (1, 8))),
    }


head_eps = 1e-05
norm_eps = 1e-06
rope_base = 10000.0

def rotate(values, places):
    half = values.shape[-1] // 2
    inverse = rope_base ** (-jnp.arange(half, dtype=jnp.float32) / half)
    angles = places[:, None] * inverse[None, :]
    cosine = jnp.cos(angles)[:, None, :]
    sine = jnp.sin(angles)[:, None, :]
    front = values[..., :half]
    back = values[..., half:]
    return jnp.concatenate([front * cosine - back * sine, back * cosine + front * sine], axis=-1)

def block_step(carried, inputs):
    query, keys, values, log_rate = inputs
    running = jnp.cumsum(log_rate, axis=0)
    spread = running[:, None, :] - running[None, :, :]
    length = log_rate.shape[0]
    lower = (jnp.arange(length)[:, None] >= jnp.arange(length)[None, :])[:, :, None]
    factor = jnp.where(lower, jnp.exp(jnp.minimum(spread, 0.0)), 0.0)
    scores = jnp.einsum('thd,shd->tsh', query, keys) * factor
    within = jnp.einsum('tsh,she->the', scores, values)
    across = jnp.einsum('thd,hde->the', query, carried) * jnp.exp(running)[:, :, None]
    tail_decay = jnp.exp(running[-1][None, :] - running)
    updated = jnp.exp(running[-1])[:, None, None] * carried + jnp.einsum('shd,she->hde', keys * tail_decay[:, :, None], values)
    return (updated, within + across)

def retain(query, keys, values, log_rate):
    length, count_of_heads, width = query.shape
    blocks = length // BLOCK

    def shaped(array):
        return array.reshape(blocks, BLOCK, count_of_heads, width)
    rates = log_rate.T.reshape(blocks, BLOCK, count_of_heads)
    carried = jnp.zeros((count_of_heads, width, width), jnp.float32)
    final_state, outputs = lax.scan(block_step, carried, (shaped(query), shaped(keys), shaped(values), rates))
    return outputs.reshape(length, count_of_heads, width)

def head_norm(values):
    centre = values - lax.optimization_barrier(jnp.mean(values, axis=-1, keepdims=True))
    spread = lax.optimization_barrier(jnp.mean(centre * centre, axis=-1, keepdims=True))
    return centre * lax.rsqrt(spread + head_eps)

def group(query, keys, values, gate, log_rate, width, places):
    length = query.shape[0]
    count_of_heads = query.shape[1] // width

    def split(array):
        return array.astype(jnp.float32).reshape(length, count_of_heads, width)
    query_rot = rotate(split(query), places)
    keys_rot = rotate(split(keys), places) * width ** (-0.5)
    normed = head_norm(retain(query_rot, keys_rot, split(values), log_rate)).reshape(length, count_of_heads * width)
    return (jax.nn.silu(gate.astype(jnp.float32)) * normed).astype(jnp.bfloat16)

def reference(stream_in, query_wide, key_wide, value_wide, gate_wide, decay_wide, query_narrow, key_narrow, value_narrow, gate_narrow, decay_narrow, output_wide, output_narrow, norm_gain, up_weight, down_weight):
    places = jnp.arange(TOKEN_POSITIONS, dtype=jnp.float32)
    mixed_wide = group(query_wide, key_wide, value_wide, gate_wide, decay_wide, HDW, places)
    mixed_narrow = group(query_narrow, key_narrow, value_narrow, gate_narrow, decay_narrow, HDN, places)
    mixed_sum = jnp.dot(mixed_wide, output_wide, preferred_element_type=jnp.float32) + jnp.dot(mixed_narrow, output_narrow, preferred_element_type=jnp.float32)
    middle = (stream_in.astype(jnp.float32) + mixed_sum).astype(jnp.bfloat16)
    middle_f = middle.astype(jnp.float32)
    normed_rows = (middle_f * lax.rsqrt(lax.optimization_barrier(jnp.mean(middle_f * middle_f, axis=-1, keepdims=True)) + norm_eps) * norm_gain.astype(jnp.float32)).astype(jnp.bfloat16)
    up_sum = jnp.dot(normed_rows, up_weight, preferred_element_type=jnp.float32)
    hidden = jnp.square(jax.nn.relu(up_sum)).astype(jnp.bfloat16)
    down_sum = jnp.dot(hidden, down_weight, preferred_element_type=jnp.float32)
    return (middle_f + down_sum).astype(jnp.bfloat16)
```

```python
import functools
import jax
import jax.numpy as jnp
import numpy as np
from jax import lax
from jax.experimental import pallas as pl
from jax.experimental.pallas import tpu as pltpu
from jax.sharding import PartitionSpec as P

HDW = 128
HDN = 64
BLOCK = 128


head_eps = 1e-05
norm_eps = 1e-06
rope_base = 10000.0


def carried_in(shard, axis, join, neutral):
    place = lax.axis_index(axis)
    gathered = jax.tree.map(
        lambda a, kind: lax.all_gather(a.astype(kind), axis),
        shard,
        (jnp.bfloat16, jnp.bfloat16, jnp.bfloat16, jnp.bfloat16),
    )
    state = jax.tree.map(lambda a, e: jnp.zeros_like(a) + jnp.asarray(e, a.dtype), shard, neutral)

    def one(turn, state):
        return join(
            state,
            jax.tree.map(
                lambda a, own: lax.dynamic_index_in_dim(a, turn, 0, False).astype(own.dtype),
                gathered,
                shard,
            ),
        )

    return lax.fori_loop(0, place, one, state)


def rotate(values, places):
    half = values.shape[-1] // 2
    inverse = rope_base ** (-jnp.arange(half, dtype=jnp.float32) / half)
    angles = places[:, None] * inverse[None, :]
    cosine = jnp.cos(angles)[:, None, :]
    sine = jnp.sin(angles)[:, None, :]
    front = values[..., :half]
    back = values[..., half:]
    return jnp.concatenate([front * cosine - back * sine, back * cosine + front * sine], axis=-1)


def block_step(carried, inputs):
    query, keys, values, log_rate = inputs
    running = jnp.cumsum(log_rate, axis=0)
    spread = running[:, None, :] - running[None, :, :]
    length = log_rate.shape[0]
    lower = (jnp.arange(length)[:, None] >= jnp.arange(length)[None, :])[:, :, None]
    factor = jnp.where(lower, jnp.exp(jnp.minimum(spread, 0.0)), 0.0)
    scores = jnp.einsum("thd,shd->tsh", query, keys) * factor
    within = jnp.einsum("tsh,she->the", scores, values)
    across = jnp.einsum("thd,hde->the", query, carried) * jnp.exp(running)[:, :, None]
    tail_decay = jnp.exp(running[-1][None, :] - running)
    updated = jnp.exp(running[-1])[:, None, None] * carried + jnp.einsum(
        "shd,she->hde", keys * tail_decay[:, :, None], values
    )
    return (updated, within + across)


def head_norm(values):
    centre = values - jnp.mean(values, axis=-1, keepdims=True)
    spread = jnp.mean(centre * centre, axis=-1, keepdims=True)
    return centre * lax.rsqrt(spread + head_eps)


def local_group(query, keys, values, log_rate, width, places):
    length = query.shape[0]
    count_of_heads = query.shape[1] // width
    blocks = length // BLOCK

    def split(array):
        return array.astype(jnp.float32).reshape(length, count_of_heads, width)

    query_rot = rotate(split(query), places)
    keys_rot = rotate(split(keys), places) * width ** (-0.5)
    rates = log_rate.T
    carried = jnp.zeros((count_of_heads, width, width), jnp.float32)
    final_state, outputs = lax.scan(
        block_step,
        carried,
        (
            query_rot.reshape(blocks, BLOCK, count_of_heads, width),
            keys_rot.reshape(blocks, BLOCK, count_of_heads, width),
            split(values).reshape(blocks, BLOCK, count_of_heads, width),
            rates.reshape(blocks, BLOCK, count_of_heads),
        ),
    )
    running = jnp.cumsum(rates, axis=0)
    return (
        query_rot,
        outputs.reshape(length, count_of_heads, width),
        final_state,
        jnp.exp(running[-1]),
        running,
    )


def finish_group(query_rot, outputs, incoming, running, gate):
    length = outputs.shape[0]
    outputs = (
        outputs + jnp.einsum("thd,hde->the", query_rot, incoming) * jnp.exp(running)[:, :, None]
    )
    normed = head_norm(outputs).reshape(length, -1)
    return (jax.nn.silu(gate.astype(jnp.float32)) * normed).astype(jnp.bfloat16)


def chain(earlier, later):
    rate_wide, memory_wide, rate_narrow, memory_narrow = earlier
    later_rate_wide, later_memory_wide, later_rate_narrow, later_memory_narrow = later
    return (
        rate_wide * later_rate_wide,
        memory_wide * later_rate_wide[:, None, None] + later_memory_wide,
        rate_narrow * later_rate_narrow,
        memory_narrow * later_rate_narrow[:, None, None] + later_memory_narrow,
    )


def row_norm(middle, norm_gain):
    middle_f = middle.astype(jnp.float32)
    scale = lax.rsqrt(jnp.mean(middle_f * middle_f, axis=-1, keepdims=True) + norm_eps)
    return (middle_f * scale * norm_gain.astype(jnp.float32)).astype(jnp.bfloat16)


def on_device(
    stream_in,
    query_wide,
    key_wide,
    value_wide,
    gate_wide,
    decay_wide,
    query_narrow,
    key_narrow,
    value_narrow,
    gate_narrow,
    decay_narrow,
    output_wide,
    output_narrow,
    norm_gain,
    up_weight,
    down_weight,
):
    length = query_wide.shape[0]
    places = (lax.axis_index("sp") * length + jnp.arange(length, dtype=jnp.int32)).astype(
        jnp.float32
    )
    wide_query, wide_out, wide_state, wide_total, wide_running = local_group(
        query_wide, key_wide, value_wide, decay_wide, HDW, places
    )
    narrow_query, narrow_out, narrow_state, narrow_total, narrow_running = local_group(
        query_narrow, key_narrow, value_narrow, decay_narrow, HDN, places
    )
    identity = (
        jnp.ones_like(wide_total),
        jnp.zeros_like(wide_state),
        jnp.ones_like(narrow_total),
        jnp.zeros_like(narrow_state),
    )
    incoming = carried_in(
        (wide_total, wide_state, narrow_total, narrow_state), "sp", chain, identity
    )
    mixed_wide = finish_group(wide_query, wide_out, incoming[1], wide_running, gate_wide)
    mixed_narrow = finish_group(narrow_query, narrow_out, incoming[3], narrow_running, gate_narrow)
    mixed_sum = lax.psum_scatter(
        (
            jnp.dot(mixed_wide, output_wide, preferred_element_type=jnp.float32)
            + jnp.dot(mixed_narrow, output_narrow, preferred_element_type=jnp.float32)
        ).astype(jnp.bfloat16),
        "tp",
        scatter_dimension=0,
        tiled=True,
    ).astype(jnp.float32)
    middle = (stream_in.astype(jnp.float32) + mixed_sum).astype(jnp.bfloat16)
    normed = lax.all_gather(row_norm(middle, norm_gain), "tp", axis=0, tiled=True)
    up_sum = jnp.dot(
        normed,
        lax.all_gather(up_weight, "sp", axis=0, tiled=True),
        preferred_element_type=jnp.float32,
    )
    hidden = jnp.square(jax.nn.relu(up_sum)).astype(jnp.bfloat16)
    down_sum = jnp.dot(
        hidden,
        lax.all_gather(down_weight, "sp", axis=1, tiled=True),
        preferred_element_type=jnp.float32,
    )
    down_rows = lax.psum_scatter(
        down_sum.astype(jnp.bfloat16), "tp", scatter_dimension=0, tiled=True
    ).astype(jnp.float32)
    return (middle.astype(jnp.float32) + down_rows).astype(jnp.bfloat16)


F32 = jnp.float32
BF16 = jnp.bfloat16
MESH_ID = pl.DeviceIdType.MESH


def turn_tables(shards, length):
    lane = np.arange(128)
    offsets, starts = [], []
    for width in (HDW, HDN):
        half = width // 2
        inverse = rope_base ** (-((lane % half).astype(np.float64)) / half)
        inside = np.arange(BLOCK)[:, None] * inverse[None, :]
        first = (np.arange(shards * length // BLOCK) * BLOCK)[:, None] * inverse[None, :]
        offsets += [np.cos(inside), np.sin(inside)]
        starts += [np.cos(first), np.sin(first)]
    return np.stack(offsets).astype(np.float32), np.stack(starts).astype(np.float32)


def dot(a, b):
    return jnp.dot(a, b, preferred_element_type=F32)


def dot_rows(a, b):
    return lax.dot_general(a, b, (((0,), (0,)), ((), ())), preferred_element_type=F32)


def dot_cols(a, b):
    return lax.dot_general(a, b, (((1,), (1,)), ((), ())), preferred_element_type=F32)


def layer_kernel(
    SP, TP,
    stream, qw, kw, vw, gw, qn, kn, vn, gn, decay, offs, starts, gain, ow_w, ow_n, up, down,
    out,
    up_buf, down_buf, ow_buf, st_in, k_rot, before, inside, mixed, mix_in, mid, rows, hidden, part, part_in,
    ssem, rsem, lsem,
):
    sp = lax.axis_index("sp")
    tp = lax.axis_index("tp")
    NZ = SP // 2
    z = sp // 2
    y = sp % 2
    T = qw.shape[0]
    NB = T // BLOCK
    RT = T // TP
    RB = up.shape[0]
    CB = down.shape[1]
    D = stream.shape[1]
    FH = up.shape[1]
    mate = tp + 1 - 2 * (tp % 2)

    def at(dz, dy):
        return ((z + dz) % NZ) * 2 + (y + dy) % 2

    count = [0]
    pending = []

    def send(src, dst, device):
        k = count[0]
        count[0] += 1
        copy = pltpu.make_async_remote_copy(
            src_ref=src, dst_ref=dst, send_sem=ssem.at[k], recv_sem=rsem.at[k],
            device_id=device, device_id_type=MESH_ID,
        )
        copy.start()
        pending.append(copy)
        return copy

    def to_sp(i):
        return (i, tp)

    def to_tp(i):
        return (sp, i)

    barrier = pltpu.get_barrier_semaphore()
    for d in range(1, SP):
        pl.semaphore_signal(barrier, inc=1, device_id=to_sp((sp + d) % SP), device_id_type=MESH_ID)
    for d in range(1, TP):
        pl.semaphore_signal(barrier, inc=1, device_id=to_tp((tp + d) % TP), device_id_type=MESH_ID)
    pl.semaphore_wait(barrier, SP + TP - 2)

    def up_at(i, lo=0, n=RB):
        return up_buf.at[pl.ds(pl.multiple_of(i * RB + lo, RB // 2), n), :]

    def down_at(i, lo=0, n=FH):
        return down_buf.at[i, pl.ds(lo, n), :]

    above, below, across_y = to_sp(at(1, 0)), to_sp(at(-1, 0)), to_sp(at(0, 1))
    a_y, a_p, a_m, b_y, b_p, c_p, c_m, d_m = ({} for _ in range(8))
    place = {"up": up_at, "down": down_at}
    own = {"up": up, "down": down}
    full = {"up": RB, "down": FH}

    def first_y(w):
        a_y[w] = send(own[w], place[w](sp), across_y)

    def first_p(w):
        a_p[w] = send(own[w], place[w](sp), above)

    def first_m(w):
        a_m[w] = send(own[w], place[w](sp), below)

    def second_y(w):
        b_y[w] = send(place[w](at(1, 0)), place[w](at(1, 0)), across_y)

    def second_p(w):
        b_p[w] = send(place[w](at(0, 1)), place[w](at(0, 1)), above)

    def half_p(w):
        h = full[w] // 2
        c_p[w] = send(place[w](at(-1, 0), 0, h), place[w](at(-1, 0), 0, h), above)

    def half_m(w):
        h = full[w] // 2
        c_m[w] = send(place[w](at(1, 0), h, h), place[w](at(1, 0), h, h), below)

    def third_m(w):
        d_m[w] = send(place[w](at(1, 1)), place[w](at(1, 1)), below)

    first_y("up")
    first_p("up")
    first_m("up")

    locals_ = []

    def keep(src, dst):
        copy = pltpu.make_async_copy(src, dst, lsem.at[len(locals_)])
        copy.start()
        locals_.append(copy)

    def ow_at(i, g):
        return ow_buf.at[i, pl.ds(g * 128, 128), :]

    ow_mate = [send(r, ow_at(tp, g), to_tp(mate)) for g, r in enumerate((ow_w, ow_n))]
    ow_far = [
        (q, g, send(r, ow_at(tp, g), to_tp((tp + 2 * q) % TP)))
        for q in range(1, TP // 2) for g, r in enumerate((ow_w, ow_n))
    ]
    keep(up, up_at(sp))
    keep(down, down_at(sp))
    keep(ow_w, ow_at(tp, 0))
    keep(ow_n, ow_at(tp, 1))

    lane = lax.broadcasted_iota(jnp.int32, (128, 128), 1)
    row = lax.broadcasted_iota(jnp.int32, (128, 128), 0)
    lower = row >= lane
    low = lane < HDN
    low_row = row < HDN
    diagonal = low == low_row
    cr = decay[...]
    step = 1
    while step < 128:
        cr = cr + jnp.where(lane >= step, pltpu.roll(cr, step, 1), 0.0)
        step *= 2
    ct = cr.T

    def col(h, b):
        return ct[:, h * NB + b:h * NB + b + 1]

    def line(h, b):
        return cr[h * NB + b:h * NB + b + 1, :]

    def total(h, b):
        return cr[h * NB + b:h * NB + b + 1, 127:128]

    def pair(a, b):
        return jnp.where(low, a, b)

    sign_w = jnp.where(low, -1.0, 1.0)
    early = (lane % HDN) < HDN // 2
    sign_n = jnp.where(early, -1.0, 1.0)

    def tables(g, b):
        cb = starts[2 * g, pl.ds(sp * NB + b, 1), :]
        sb = starts[2 * g + 1, pl.ds(sp * NB + b, 1), :]
        co, so = offs[2 * g], offs[2 * g + 1]
        return co * cb - so * sb, (so * cb + co * sb) * (sign_n if g else sign_w)

    def turned(x, table, g):
        if g:
            other = jnp.where(early, pltpu.roll(x, 128 - HDN // 2, 1), pltpu.roll(x, HDN // 2, 1))
        else:
            other = pltpu.roll(x, HDW // 2, 1)
        return x * table[0] + other * table[1]

    state_w = jnp.zeros((128, 128), F32)
    state_n = jnp.zeros((128, 128), F32)
    sums = [jnp.zeros((1, 1), F32) for _ in range(3)]
    for b in range(NB):
        rs = pl.ds(b * BLOCK, BLOCK)
        before[0, b] = state_w
        before[1, b] = state_n
        kwr = turned(kw[rs, :].astype(F32), tables(0, b), 0) * HDW ** (-0.5)
        knr = turned(kn[rs, :].astype(F32), tables(1, b), 1) * HDN ** (-0.5)
        k_rot[rs, 0:128] = kwr.astype(BF16)
        k_rot[rs, 128:256] = knr.astype(BF16)
        t0, t1, t2 = total(0, b), total(1, b), total(2, b)
        sums = [s + t for s, t in zip(sums, (t0, t1, t2))]
        tail_w = jnp.exp(t0 - col(0, b))
        tail_n = pair(jnp.exp(t1 - col(1, b)), jnp.exp(t2 - col(2, b)))
        state_w = jnp.exp(t0) * state_w + dot_rows((kwr * tail_w).astype(BF16), vw[rs, :])
        grown = dot_rows((knr * tail_n).astype(BF16), vn[rs, :])
        state_n = jnp.where(low_row, jnp.exp(t1), jnp.exp(t2)) * state_n + jnp.where(diagonal, grown, 0.0)
    small = lax.broadcasted_iota(jnp.int32, (16, 128), 0)
    rates = jnp.where(small == 0, jnp.exp(sums[0]), jnp.where(small == 1, jnp.exp(sums[1]), jnp.exp(sums[2])))
    st_in[sp, 0:128, :] = state_w.astype(BF16)
    st_in[sp, 128:256, :] = state_n.astype(BF16)
    st_in[sp, 256:272, :] = rates.astype(BF16)
    states = [send(st_in.at[sp], st_in.at[sp], to_sp((sp + d) % SP)) for d in range(1, SP)]

    for b in range(NB):
        rs = pl.ds(b * BLOCK, BLOCK)
        kwr, knr = k_rot[rs, 0:128], k_rot[rs, 128:256]
        qwr = turned(qw[rs, :].astype(F32), tables(0, b), 0)
        qnr = turned(qn[rs, :].astype(F32), tables(1, b), 1)

        def factor(h):
            return jnp.where(lower, jnp.exp(jnp.minimum(col(h, b) - line(h, b), 0.0)), 0.0)

        scores = (dot_cols(qwr.astype(BF16), kwr) * factor(0)).astype(BF16)
        inside[rs, 0:128] = dot(scores, vw[rs, :])
        near = (dot_cols(jnp.where(low, qnr, 0.0).astype(BF16), knr) * factor(1)).astype(BF16)
        far = (dot_cols(jnp.where(low, 0.0, qnr).astype(BF16), knr) * factor(2)).astype(BF16)
        inside[rs, 128:256] = pair(dot(near, vn[rs, :]), dot(far, vn[rs, :]))
        k_rot[rs, 0:128] = (qwr * jnp.exp(col(0, b))).astype(BF16)
        k_rot[rs, 128:256] = (qnr * pair(jnp.exp(col(1, b)), jnp.exp(col(2, b)))).astype(BF16)

    a_y["up"].wait_recv()
    a_p["up"].wait_recv()
    a_m["up"].wait_recv()
    second_y("up")
    first_y("down")
    second_p("up")
    half_p("up")
    first_p("down")
    half_m("up")
    first_m("down")

    for copy in states:
        copy.wait_recv()
    s_w = jnp.zeros((128, 128), F32)
    s_n = jnp.zeros((128, 128), F32)
    for j in range(SP):
        r = st_in[j, 256:272, :].astype(F32)
        s_w = jnp.where(j < sp, s_w * r[0:1, :] + st_in[j, 0:128, :].astype(F32), s_w)
        s_n = jnp.where(
            j < sp, s_n * jnp.where(low_row, r[1:2, :], r[2:3, :]) + st_in[j, 128:256, :].astype(F32), s_n
        )

    sums = [jnp.zeros((1, 1), F32) for _ in range(3)]
    for b in range(NB):
        rs = pl.ds(b * BLOCK, BLOCK)
        whole_w = before[0, b] + jnp.exp(sums[0]) * s_w
        whole_n = before[1, b] + jnp.where(low_row, jnp.exp(sums[1]), jnp.exp(sums[2])) * s_n
        sums = [s + total(h, b) for h, s in enumerate(sums)]
        o_w = inside[rs, 0:128] + dot(k_rot[rs, 0:128], whole_w.astype(BF16))
        o_n = inside[rs, 128:256] + dot(k_rot[rs, 128:256], whole_n.astype(BF16))

        def both(x):
            first = jnp.sum(jnp.where(low, x, 0.0), axis=-1, keepdims=True) / HDN
            second = jnp.sum(jnp.where(low, 0.0, x), axis=-1, keepdims=True) / HDN
            return pair(first, second)

        c_w = o_w - jnp.mean(o_w, axis=-1, keepdims=True)
        n_w = c_w * lax.rsqrt(jnp.mean(c_w * c_w, axis=-1, keepdims=True) + head_eps)
        c_n = o_n - both(o_n)
        n_n = c_n * lax.rsqrt(both(c_n * c_n) + head_eps)
        mixed[rs, 0:128] = (jax.nn.silu(gw[rs, :].astype(F32)) * n_w).astype(BF16)
        mixed[rs, 128:256] = (jax.nn.silu(gn[rs, :].astype(F32)) * n_n).astype(BF16)

    def my_rows(i):
        return pl.ds(pl.multiple_of(i * RT, RT), RT)

    swaps = [
        send(mixed.at[my_rows((tp + d) % TP), :], mix_in.at[tp], to_tp((tp + d) % TP)) for d in range(1, TP)
    ]
    mix_in[tp] = mixed[my_rows(tp), :]
    ow_relay = []
    for q, g, copy in ow_far:
        copy.wait_recv()
        came = (tp + TP - 2 * q) % TP
        ow_relay.append(send(ow_at(came, g), ow_at(came, g), to_tp(mate)))
    b_y["up"].wait_recv()
    third_m("up")
    for copy in swaps + ow_mate + ow_relay:
        copy.wait_recv()
    for copy in locals_:
        copy.wait()

    def project(c, _):
        cs = pl.ds(pl.multiple_of(c * 512, 512), 512)
        acc = stream[:, cs].astype(F32)
        for i in range(TP):
            acc = acc + dot(mix_in[i], ow_buf[i, :, cs])
        mid[:, cs] = acc.astype(BF16)
        return 0

    lax.fori_loop(0, D // 512, project, 0)

    def norm(i, _):
        m = mid[pl.ds(pl.multiple_of(i * 32, 32), 32), :].astype(F32)
        scale = lax.rsqrt(jnp.mean(m * m, axis=-1, keepdims=True) + norm_eps)
        rows[pl.ds(pl.multiple_of(tp * RT + i * 32, 32), 32), :] = (m * scale * gain[...].astype(F32)).astype(BF16)
        return 0

    lax.fori_loop(0, RT // 32, norm, 0)
    mine = rows.at[my_rows(tp), :]
    row_far = [(q, send(mine, mine, to_tp((tp + 2 * q) % TP))) for q in range(1, TP // 2)]
    row_mate = send(mine, mine, to_tp(mate))

    a_m["down"].wait_recv()
    second_y("down")
    half_m("down")
    row_relay = []
    for q, copy in row_far:
        copy.wait_recv()
        came = rows.at[my_rows((tp + TP - 2 * q) % TP), :]
        row_relay.append((q, send(came, came, to_tp(mate))))
    a_y["down"].wait_recv()
    second_p("down")
    for c in (b_p, c_p, c_m, d_m):
        c["up"].wait_recv()
    a_p["down"].wait_recv()
    half_p("down")
    row_mate.wait_recv()

    def up_rows(i):
        rs = pl.ds(pl.multiple_of(i * 2 * RT, 2 * RT), 2 * RT)

        def one(c, _):
            cs = pl.ds(pl.multiple_of(c * 512, 512), 512)
            h = jnp.maximum(dot(rows[rs, :], up_buf[:, cs]), 0.0)
            hidden[rs, cs] = (h * h).astype(BF16)
            return 0

        lax.fori_loop(0, FH // 512, one, 0)

    up_rows(tp // 2)
    for q, copy in row_relay:
        copy.wait_recv()
        up_rows(((tp + TP - 2 * q) % TP) // 2)

    def chunk(k, j):
        def one(i, _):
            rs = pl.ds(pl.multiple_of(i * 2 * RT, 2 * RT), 2 * RT)
            part[k, rs, :] = dot(hidden[rs, :], down_buf[j]).astype(BF16)
            return 0

        lax.fori_loop(0, TP // 2, one, 0)
        return [
            send(part.at[k, my_rows((tp + d) % TP), :], part_in.at[k, d - 1], to_tp((tp + d) % TP))
            for d in range(1, TP)
        ]

    def finish(k, j, copies):
        for copy in copies:
            copy.wait_recv()
        cs = pl.ds(pl.multiple_of(j * CB, CB), CB)
        acc = mid[:, cs].astype(F32) + part[k, my_rows(tp), :].astype(F32)
        for d in range(TP - 1):
            acc = acc + part_in[k, d].astype(F32)
        out[:, cs] = acc.astype(BF16)

    order = [
        (at(0, 0), []), (at(1, 0), []), (at(0, 1), []), (at(-1, 0), []),
        (at(1, 1), [b_y]), (at(2, 0), [c_p, c_m]), (at(-1, 1), [b_p]), (at(2, 1), [d_m]),
    ]
    done = []
    for k, (j, needs) in enumerate(order):
        for c in needs:
            c["down"].wait_recv()
            if c is b_y:
                third_m("down")
        done.append((k, j, chunk(k, j)))
        if k:
            finish(*done[k - 1])
    finish(*done[-1])
    for copy in pending:
        copy.wait_send()


def one_kernel(SP, TP, *args):
    (stream, qw, kw, vw, gw, dw, qn, kn, vn, gn, dn, ow, on, gain, up, down) = args
    T = qw.shape[0]
    NB = T // BLOCK
    D = stream.shape[1]
    RT = T // TP
    FH = up.shape[1]
    CB = down.shape[1]
    heads = dw.shape[0] + dn.shape[0]
    decay = jnp.concatenate([dw, dn]).reshape(heads * NB, BLOCK)
    decay = jnp.pad(decay, ((0, 128 - heads * NB), (0, 0)))
    offs, starts = turn_tables(SP, T)
    vmem = pl.BlockSpec(memory_space=pltpu.VMEM)
    hbm = pl.BlockSpec(memory_space=pl.ANY)
    copies = 72
    return pl.pallas_call(
        functools.partial(layer_kernel, SP, TP),
        out_shape=jax.ShapeDtypeStruct((RT, D), BF16),
        in_specs=[vmem] * 13 + [hbm] * 4,
        out_specs=vmem,
        scratch_shapes=[
            pltpu.VMEM((D, FH), BF16),
            pltpu.VMEM((SP, FH, CB), BF16),
            pltpu.VMEM((TP, 256, D), BF16),
            pltpu.VMEM((SP, 272, 128), BF16),
            pltpu.VMEM((T, 256), BF16),
            pltpu.VMEM((2, NB, 128, 128), F32),
            pltpu.VMEM((T, 256), F32),
            pltpu.VMEM((T, 256), BF16),
            pltpu.VMEM((TP, RT, 256), BF16),
            pltpu.VMEM((RT, D), BF16),
            pltpu.VMEM((T, D), BF16),
            pltpu.VMEM((T, FH), BF16),
            pltpu.VMEM((SP, T, CB), BF16),
            pltpu.VMEM((SP, TP - 1, RT, CB), BF16),
            pltpu.SemaphoreType.DMA((copies,)),
            pltpu.SemaphoreType.DMA((copies,)),
            pltpu.SemaphoreType.DMA((4,)),
        ],
        compiler_params=pltpu.CompilerParams(
            collective_id=0, has_side_effects=True, vmem_limit_bytes=60 * 1024 * 1024
        ),
    )(stream, qw, kw, vw, gw, qn, kn, vn, gn, decay, jnp.asarray(offs), jnp.asarray(starts),
      gain.reshape(1, D), ow, on, up, down)


def fits_kernel(SP, TP, args):
    D, FF = args[14].shape
    T = args[1].shape[0] // SP
    return (
        SP == 8 and TP == 4 and D % (SP * 128) == 0 and T % (TP * 32) == 0 and T % BLOCK == 0
        and args[1].shape[1] == TP * 128 and args[6].shape[1] == TP * 128
    )


def solution(mesh):
    in_specs = (
        P(("sp", "tp"), None),
        P("sp", "tp"),
        P("sp", "tp"),
        P("sp", "tp"),
        P("sp", "tp"),
        P("tp", "sp"),
        P("sp", "tp"),
        P("sp", "tp"),
        P("sp", "tp"),
        P("sp", "tp"),
        P("tp", "sp"),
        P("tp", None),
        P("tp", None),
        P(),
        P("sp", "tp"),
        P("tp", "sp"),
    )
    out_specs = P(("sp", "tp"), None)
    SP, TP = mesh.shape["sp"], mesh.shape["tp"]

    def layer(*args):
        body = functools.partial(one_kernel, SP, TP) if fits_kernel(SP, TP, args) else on_device
        return jax.shard_map(
            body, mesh=mesh, in_specs=in_specs, out_specs=out_specs, check_vma=False
        )(*args)

    return layer
```

```python
import functools
import jax
import jax.numpy as jnp
import numpy as np
from jax import lax
from jax.experimental import pallas as pl
from jax.experimental.pallas import tpu as pltpu
from jax.sharding import PartitionSpec as P

HDW = 128
HDN = 64
BLOCK = 128


head_eps = 1e-05
norm_eps = 1e-06
rope_base = 10000.0


def carried_in(shard, axis, join, neutral):
    place = lax.axis_index(axis)
    gathered = jax.tree.map(
        lambda a, kind: lax.all_gather(a.astype(kind), axis),
        shard,
        (jnp.bfloat16, jnp.bfloat16, jnp.bfloat16, jnp.bfloat16),
    )
    state = jax.tree.map(lambda a, e: jnp.zeros_like(a) + jnp.asarray(e, a.dtype), shard, neutral)

    def one(turn, state):
        return join(
            state,
            jax.tree.map(
                lambda a, own: lax.dynamic_index_in_dim(a, turn, 0, False).astype(own.dtype),
                gathered,
                shard,
            ),
        )

    return lax.fori_loop(0, place, one, state)


def rotate(values, places):
    half = values.shape[-1] // 2
    inverse = rope_base ** (-jnp.arange(half, dtype=jnp.float32) / half)
    angles = places[:, None] * inverse[None, :]
    cosine = jnp.cos(angles)[:, None, :]
    sine = jnp.sin(angles)[:, None, :]
    front = values[..., :half]
    back = values[..., half:]
    return jnp.concatenate([front * cosine - back * sine, back * cosine + front * sine], axis=-1)


def block_step(carried, inputs):
    query, keys, values, log_rate = inputs
    running = jnp.cumsum(log_rate, axis=0)
    spread = running[:, None, :] - running[None, :, :]
    length = log_rate.shape[0]
    lower = (jnp.arange(length)[:, None] >= jnp.arange(length)[None, :])[:, :, None]
    factor = jnp.where(lower, jnp.exp(jnp.minimum(spread, 0.0)), 0.0)
    scores = jnp.einsum("thd,shd->tsh", query, keys) * factor
    within = jnp.einsum("tsh,she->the", scores, values)
    across = jnp.einsum("thd,hde->the", query, carried) * jnp.exp(running)[:, :, None]
    tail_decay = jnp.exp(running[-1][None, :] - running)
    updated = jnp.exp(running[-1])[:, None, None] * carried + jnp.einsum(
        "shd,she->hde", keys * tail_decay[:, :, None], values
    )
    return (updated, within + across)


def head_norm(values):
    centre = values - jnp.mean(values, axis=-1, keepdims=True)
    spread = jnp.mean(centre * centre, axis=-1, keepdims=True)
    return centre * lax.rsqrt(spread + head_eps)


def local_group(query, keys, values, log_rate, width, places):
    length = query.shape[0]
    count_of_heads = query.shape[1] // width
    blocks = length // BLOCK

    def split(array):
        return array.astype(jnp.float32).reshape(length, count_of_heads, width)

    query_rot = rotate(split(query), places)
    keys_rot = rotate(split(keys), places) * width ** (-0.5)
    rates = log_rate.T
    carried = jnp.zeros((count_of_heads, width, width), jnp.float32)
    final_state, outputs = lax.scan(
        block_step,
        carried,
        (
            query_rot.reshape(blocks, BLOCK, count_of_heads, width),
            keys_rot.reshape(blocks, BLOCK, count_of_heads, width),
            split(values).reshape(blocks, BLOCK, count_of_heads, width),
            rates.reshape(blocks, BLOCK, count_of_heads),
        ),
    )
    running = jnp.cumsum(rates, axis=0)
    return (
        query_rot,
        outputs.reshape(length, count_of_heads, width),
        final_state,
        jnp.exp(running[-1]),
        running,
    )


def finish_group(query_rot, outputs, incoming, running, gate):
    length = outputs.shape[0]
    outputs = (
        outputs + jnp.einsum("thd,hde->the", query_rot, incoming) * jnp.exp(running)[:, :, None]
    )
    normed = head_norm(outputs).reshape(length, -1)
    return (jax.nn.silu(gate.astype(jnp.float32)) * normed).astype(jnp.bfloat16)


def chain(earlier, later):
    rate_wide, memory_wide, rate_narrow, memory_narrow = earlier
    later_rate_wide, later_memory_wide, later_rate_narrow, later_memory_narrow = later
    return (
        rate_wide * later_rate_wide,
        memory_wide * later_rate_wide[:, None, None] + later_memory_wide,
        rate_narrow * later_rate_narrow,
        memory_narrow * later_rate_narrow[:, None, None] + later_memory_narrow,
    )


def row_norm(middle, norm_gain):
    middle_f = middle.astype(jnp.float32)
    scale = lax.rsqrt(jnp.mean(middle_f * middle_f, axis=-1, keepdims=True) + norm_eps)
    return (middle_f * scale * norm_gain.astype(jnp.float32)).astype(jnp.bfloat16)


def on_device(
    stream_in,
    query_wide,
    key_wide,
    value_wide,
    gate_wide,
    decay_wide,
    query_narrow,
    key_narrow,
    value_narrow,
    gate_narrow,
    decay_narrow,
    output_wide,
    output_narrow,
    norm_gain,
    up_weight,
    down_weight,
):
    length = query_wide.shape[0]
    places = (lax.axis_index("sp") * length + jnp.arange(length, dtype=jnp.int32)).astype(
        jnp.float32
    )
    wide_query, wide_out, wide_state, wide_total, wide_running = local_group(
        query_wide, key_wide, value_wide, decay_wide, HDW, places
    )
    narrow_query, narrow_out, narrow_state, narrow_total, narrow_running = local_group(
        query_narrow, key_narrow, value_narrow, decay_narrow, HDN, places
    )
    identity = (
        jnp.ones_like(wide_total),
        jnp.zeros_like(wide_state),
        jnp.ones_like(narrow_total),
        jnp.zeros_like(narrow_state),
    )
    incoming = carried_in(
        (wide_total, wide_state, narrow_total, narrow_state), "sp", chain, identity
    )
    mixed_wide = finish_group(wide_query, wide_out, incoming[1], wide_running, gate_wide)
    mixed_narrow = finish_group(narrow_query, narrow_out, incoming[3], narrow_running, gate_narrow)
    mixed_sum = lax.psum_scatter(
        (
            jnp.dot(mixed_wide, output_wide, preferred_element_type=jnp.float32)
            + jnp.dot(mixed_narrow, output_narrow, preferred_element_type=jnp.float32)
        ).astype(jnp.bfloat16),
        "tp",
        scatter_dimension=0,
        tiled=True,
    ).astype(jnp.float32)
    middle = (stream_in.astype(jnp.float32) + mixed_sum).astype(jnp.bfloat16)
    normed = lax.all_gather(row_norm(middle, norm_gain), "tp", axis=0, tiled=True)
    up_sum = jnp.dot(
        normed,
        lax.all_gather(up_weight, "sp", axis=0, tiled=True),
        preferred_element_type=jnp.float32,
    )
    hidden = jnp.square(jax.nn.relu(up_sum)).astype(jnp.bfloat16)
    down_sum = jnp.dot(
        hidden,
        lax.all_gather(down_weight, "sp", axis=1, tiled=True),
        preferred_element_type=jnp.float32,
    )
    down_rows = lax.psum_scatter(
        down_sum.astype(jnp.bfloat16), "tp", scatter_dimension=0, tiled=True
    ).astype(jnp.float32)
    return (middle.astype(jnp.float32) + down_rows).astype(jnp.bfloat16)


F32 = jnp.float32
BF16 = jnp.bfloat16
MESH_ID = pl.DeviceIdType.MESH


def turn_tables(shards, length):
    lane = np.arange(128)
    offsets, starts = [], []
    for width in (HDW, HDN):
        half = width // 2
        inverse = rope_base ** (-((lane % half).astype(np.float64)) / half)
        inside = np.arange(BLOCK)[:, None] * inverse[None, :]
        first = (np.arange(shards * length // BLOCK) * BLOCK)[:, None] * inverse[None, :]
        offsets += [np.cos(inside), np.sin(inside)]
        starts += [np.cos(first), np.sin(first)]
    return np.stack(offsets).astype(np.float32), np.stack(starts).astype(np.float32)


def dot(a, b):
    return jnp.dot(a, b, preferred_element_type=F32)


def dot_rows(a, b):
    return lax.dot_general(a, b, (((0,), (0,)), ((), ())), preferred_element_type=F32)


def dot_cols(a, b):
    return lax.dot_general(a, b, (((1,), (1,)), ((), ())), preferred_element_type=F32)


def layer_kernel(
    SP, TP,
    stream, qw, kw, vw, gw, qn, kn, vn, gn, decay, offs, starts, gain, ow_w, ow_n, up, down,
    out,
    up_buf, down_buf, ow_buf, st_in, k_rot, before, inside, mixed, mix_in, mid, rows, hidden, part, part_in,
    ssem, rsem, lsem, zsend, zrecv,
):
    sp = lax.axis_index("sp")
    tp = lax.axis_index("tp")
    NZ = SP // 2
    z = sp // 2
    y = sp % 2
    T = qw.shape[0]
    NB = T // BLOCK
    RT = T // TP
    RB = up.shape[0]
    CB = down.shape[1]
    D = stream.shape[1]
    FH = up.shape[1] // 2
    mate = tp + 1 - 2 * (tp % 2)

    def at(dz, dy):
        return ((z + dz) % NZ) * 2 + (y + dy) % 2

    count = [0]
    pending = []

    def send(src, dst, device):
        k = count[0]
        count[0] += 1
        copy = pltpu.make_async_remote_copy(
            src_ref=src, dst_ref=dst, send_sem=ssem.at[k], recv_sem=rsem.at[k],
            device_id=device, device_id_type=MESH_ID,
        )
        copy.start()
        pending.append(copy)
        return copy

    def group(dy, dt):
        return (z * 2 + (y + dy) % 2, (tp + dt) % TP)

    def to_sp(i):
        return (i, tp)

    def to_tp(i):
        return (sp, i)

    barrier = pltpu.get_barrier_semaphore()
    for d in range(1, SP):
        pl.semaphore_signal(barrier, inc=1, device_id=to_sp((sp + d) % SP), device_id_type=MESH_ID)
    for d in range(1, TP):
        pl.semaphore_signal(barrier, inc=1, device_id=to_tp((tp + d) % TP), device_id_type=MESH_ID)
    for d in range(1, TP):
        pl.semaphore_signal(barrier, inc=1, device_id=group(1, d), device_id_type=MESH_ID)
    pl.semaphore_wait(barrier, SP + 2 * TP - 3)

    def up_at(i):
        return up_buf.at[pl.ds(pl.multiple_of(i * RB, RB), RB), :]

    def down_at(i):
        return down_buf.at[i]

    place = (up_at, down_at)

    def hidden_half(w, half):
        cut = pl.ds(pl.multiple_of(half * FH, FH), FH)
        return up.at[:, cut] if w == 0 else down.at[cut, :]

    across_y = to_sp(at(0, 1))
    line_waits = []

    def piece(w, dy, zs):
        return place[w](zs * 2 + (y + dy) % 2)

    def line_copy(w, dy, zs, src, slot, device_z):
        return pltpu.make_async_remote_copy(
            src_ref=src, dst_ref=piece(w, dy, zs), send_sem=zsend.at[slot],
            recv_sem=zrecv.at[(w * 2 + dy) * NZ + zs],
            device_id=to_sp(device_z * 2 + y), device_id_type=MESH_ID,
        )

    def line_start(when, copy):
        @pl.when(when)
        def _():
            copy.start()

        line_waits.append((when, copy))

    def line_send(w, dy):
        for t in (1, 2, 0, 3):
            src = hidden_half(w, y) if dy == 0 else piece(w, dy, z)
            far = ((z == 0) & (t == 3)) | ((z == NZ - 1) & (t == 0))
            line_start((z != t) & jnp.logical_not(far), line_copy(w, dy, z, src, (w * 2 + dy) * 5 + t, t))

    def line_wait(w, dy, zs):
        line_copy(w, dy, zs, piece(w, dy, zs), 0, (z + 1) % NZ).wait_recv()

    def line_relay(w, dy):
        for me, source, target in ((2, 0, 3), (1, 3, 0)):
            @pl.when(z == me)
            def _():
                line_wait(w, dy, source)

            slot = (w * 2 + dy) * 5 + 4
            line_start(z == me, line_copy(w, dy, source, piece(w, dy, source), slot, target))

    def line_arrived(w, dy, d):
        zs = (z + d * (1 + 2 * (z // 2))) % NZ
        relayed = ((z == 2) & (zs == 0)) | ((z == 1) & (zs == 3))

        @pl.when(jnp.logical_not(relayed))
        def _():
            line_wait(w, dy, zs)

        return zs * 2 + (y + dy) % 2

    up_y = send(hidden_half(0, (y + 1) % 2), up_at(sp), across_y)
    line_send(0, 0)

    locals_ = []

    def keep(src, dst):
        copy = pltpu.make_async_copy(src, dst, lsem.at[len(locals_)])
        copy.start()
        locals_.append(copy)

    def ow_at(i, g):
        return ow_buf.at[i, pl.ds(g * 128, 128), :]

    ow_mate = [send(r, ow_at(tp, g), to_tp(mate)) for g, r in enumerate((ow_w, ow_n))]
    ow_far = [
        (q, g, send(r, ow_at(tp, g), to_tp((tp + 2 * q) % TP)))
        for q in range(1, TP // 2) for g, r in enumerate((ow_w, ow_n))
    ]
    keep(hidden_half(0, y), up_at(sp))
    keep(hidden_half(1, y), down_at(sp))
    keep(ow_w, ow_at(tp, 0))
    keep(ow_n, ow_at(tp, 1))

    lane = lax.broadcasted_iota(jnp.int32, (128, 128), 1)
    row = lax.broadcasted_iota(jnp.int32, (128, 128), 0)
    lower = row >= lane
    low = lane < HDN
    low_row = row < HDN
    diagonal = low == low_row
    cr = decay[...]
    step = 1
    while step < 128:
        cr = cr + jnp.where(lane >= step, pltpu.roll(cr, step, 1), 0.0)
        step *= 2
    ct = cr.T

    def col(h, b):
        return ct[:, h * NB + b:h * NB + b + 1]

    def line(h, b):
        return cr[h * NB + b:h * NB + b + 1, :]

    def total(h, b):
        return cr[h * NB + b:h * NB + b + 1, 127:128]

    def pair(a, b):
        return jnp.where(low, a, b)

    sign_w = jnp.where(low, -1.0, 1.0)
    early = (lane % HDN) < HDN // 2
    sign_n = jnp.where(early, -1.0, 1.0)

    def tables(g, b):
        cb = starts[2 * g, pl.ds(sp * NB + b, 1), :]
        sb = starts[2 * g + 1, pl.ds(sp * NB + b, 1), :]
        co, so = offs[2 * g], offs[2 * g + 1]
        return co * cb - so * sb, (so * cb + co * sb) * (sign_n if g else sign_w)

    def turned(x, table, g):
        if g:
            other = jnp.where(early, pltpu.roll(x, 128 - HDN // 2, 1), pltpu.roll(x, HDN // 2, 1))
        else:
            other = pltpu.roll(x, HDW // 2, 1)
        return x * table[0] + other * table[1]

    state_w = jnp.zeros((128, 128), F32)
    state_n = jnp.zeros((128, 128), F32)
    sums = [jnp.zeros((1, 1), F32) for _ in range(3)]
    for b in range(NB):
        rs = pl.ds(b * BLOCK, BLOCK)
        before[0, b] = state_w
        before[1, b] = state_n
        kwr = turned(kw[rs, :].astype(F32), tables(0, b), 0) * HDW ** (-0.5)
        knr = turned(kn[rs, :].astype(F32), tables(1, b), 1) * HDN ** (-0.5)
        k_rot[rs, 0:128] = kwr.astype(BF16)
        k_rot[rs, 128:256] = knr.astype(BF16)
        t0, t1, t2 = total(0, b), total(1, b), total(2, b)
        sums = [s + t for s, t in zip(sums, (t0, t1, t2))]
        tail_w = jnp.exp(t0 - col(0, b))
        tail_n = pair(jnp.exp(t1 - col(1, b)), jnp.exp(t2 - col(2, b)))
        state_w = jnp.exp(t0) * state_w + dot_rows((kwr * tail_w).astype(BF16), vw[rs, :])
        grown = dot_rows((knr * tail_n).astype(BF16), vn[rs, :])
        state_n = jnp.where(low_row, jnp.exp(t1), jnp.exp(t2)) * state_n + jnp.where(diagonal, grown, 0.0)
    small = lax.broadcasted_iota(jnp.int32, (16, 128), 0)
    rates = jnp.where(small == 0, jnp.exp(sums[0]), jnp.where(small == 1, jnp.exp(sums[1]), jnp.exp(sums[2])))
    st_in[sp, 0:128, :] = state_w.astype(BF16)
    st_in[sp, 128:256, :] = state_n.astype(BF16)
    st_in[sp, 256:272, :] = rates.astype(BF16)
    states = [send(st_in.at[sp], st_in.at[sp], to_sp((sp + d) % SP)) for d in range(1, SP)]

    for b in range(NB):
        rs = pl.ds(b * BLOCK, BLOCK)
        kwr, knr = k_rot[rs, 0:128], k_rot[rs, 128:256]
        qwr = turned(qw[rs, :].astype(F32), tables(0, b), 0)
        qnr = turned(qn[rs, :].astype(F32), tables(1, b), 1)

        def factor(h):
            return jnp.where(lower, jnp.exp(jnp.minimum(col(h, b) - line(h, b), 0.0)), 0.0)

        scores = (dot_cols(qwr.astype(BF16), kwr) * factor(0)).astype(BF16)
        inside[rs, 0:128] = dot(scores, vw[rs, :])
        near = (dot_cols(jnp.where(low, qnr, 0.0).astype(BF16), knr) * factor(1)).astype(BF16)
        far = (dot_cols(jnp.where(low, 0.0, qnr).astype(BF16), knr) * factor(2)).astype(BF16)
        inside[rs, 128:256] = pair(dot(near, vn[rs, :]), dot(far, vn[rs, :]))
        k_rot[rs, 0:128] = (qwr * jnp.exp(col(0, b))).astype(BF16)
        k_rot[rs, 128:256] = (qnr * pair(jnp.exp(col(1, b)), jnp.exp(col(2, b)))).astype(BF16)

    up_y.wait_recv()
    line_send(0, 1)
    down_y = send(hidden_half(1, (y + 1) % 2), down_at(sp), across_y)
    line_send(1, 0)

    for copy in states:
        copy.wait_recv()
    s_w = jnp.zeros((128, 128), F32)
    s_n = jnp.zeros((128, 128), F32)
    for j in range(SP):
        r = st_in[j, 256:272, :].astype(F32)
        s_w = jnp.where(j < sp, s_w * r[0:1, :] + st_in[j, 0:128, :].astype(F32), s_w)
        s_n = jnp.where(
            j < sp, s_n * jnp.where(low_row, r[1:2, :], r[2:3, :]) + st_in[j, 128:256, :].astype(F32), s_n
        )

    sums = [jnp.zeros((1, 1), F32) for _ in range(3)]
    for b in range(NB):
        rs = pl.ds(b * BLOCK, BLOCK)
        whole_w = before[0, b] + jnp.exp(sums[0]) * s_w
        whole_n = before[1, b] + jnp.where(low_row, jnp.exp(sums[1]), jnp.exp(sums[2])) * s_n
        sums = [s + total(h, b) for h, s in enumerate(sums)]
        o_w = inside[rs, 0:128] + dot(k_rot[rs, 0:128], whole_w.astype(BF16))
        o_n = inside[rs, 128:256] + dot(k_rot[rs, 128:256], whole_n.astype(BF16))

        def both(x):
            first = jnp.sum(jnp.where(low, x, 0.0), axis=-1, keepdims=True) / HDN
            second = jnp.sum(jnp.where(low, 0.0, x), axis=-1, keepdims=True) / HDN
            return pair(first, second)

        c_w = o_w - jnp.mean(o_w, axis=-1, keepdims=True)
        n_w = c_w * lax.rsqrt(jnp.mean(c_w * c_w, axis=-1, keepdims=True) + head_eps)
        c_n = o_n - both(o_n)
        n_n = c_n * lax.rsqrt(both(c_n * c_n) + head_eps)
        mixed[rs, 0:128] = (jax.nn.silu(gw[rs, :].astype(F32)) * n_w).astype(BF16)
        mixed[rs, 128:256] = (jax.nn.silu(gn[rs, :].astype(F32)) * n_n).astype(BF16)

    def my_rows(i):
        return pl.ds(pl.multiple_of(i * RT, RT), RT)

    swaps = [
        send(mixed.at[my_rows((tp + d) % TP), :], mix_in.at[tp], to_tp((tp + d) % TP)) for d in range(1, TP)
    ]
    mix_in[tp] = mixed[my_rows(tp), :]
    ow_relay = []
    for q, g, copy in ow_far:
        copy.wait_recv()
        came = (tp + TP - 2 * q) % TP
        ow_relay.append(send(ow_at(came, g), ow_at(came, g), to_tp(mate)))
    line_relay(0, 0)
    for copy in swaps + ow_mate + ow_relay:
        copy.wait_recv()
    for copy in locals_:
        copy.wait()

    def project(c, _):
        cs = pl.ds(pl.multiple_of(c * 512, 512), 512)
        acc = stream[:, cs].astype(F32)
        for i in range(TP):
            acc = acc + dot(mix_in[i], ow_buf[i, :, cs])
        mid[:, cs] = acc.astype(BF16)
        return 0

    lax.fori_loop(0, D // 512, project, 0)

    def norm(i, _):
        m = mid[pl.ds(pl.multiple_of(i * 32, 32), 32), :].astype(F32)
        scale = lax.rsqrt(jnp.mean(m * m, axis=-1, keepdims=True) + norm_eps)
        rows[pl.ds(pl.multiple_of((y * TP + tp) * RT + i * 32, 32), 32), :] = (m * scale * gain[...].astype(F32)).astype(BF16)
        return 0

    lax.fori_loop(0, RT // 32, norm, 0)

    def block(dy, dt):
        return rows.at[my_rows((y + dy) % 2 * TP + (tp + dt) % TP), :]

    near_x = send(block(0, 0), block(0, 0), group(0, 2))
    near_y = send(block(0, 0), block(0, 0), group(1, 0))
    hand = [send(block(0, 0), block(0, 0), to_tp(mate))]
    line_relay(0, 1)
    down_y.wait_recv()
    line_send(1, 1)
    near_x.wait_recv()
    corner = send(block(0, 2), block(0, 2), group(1, 0))
    hand.append(send(block(0, 2), block(0, 2), to_tp(mate)))
    near_y.wait_recv()
    hand.append(send(block(1, 0), block(1, 0), to_tp(mate)))
    for dy in range(2):
        for d in range(1, NZ):
            line_arrived(0, dy, d)

    def up_rows(dy, dp):
        i = (y + dy) % 2 * (TP // 2) + (tp // 2 + dp) % (TP // 2)
        rs = pl.ds(pl.multiple_of(i * 2 * RT, 2 * RT), 2 * RT)

        def one(c, _):
            cs = pl.ds(pl.multiple_of(c * 512, 512), 512)
            h = jnp.maximum(dot(rows[rs, :], up_buf[:, cs]), 0.0)
            hidden[rs, cs] = (h * h).astype(BF16)
            return 0

        lax.fori_loop(0, FH // 512, one, 0)

    hand[0].wait_recv()
    up_rows(0, 0)
    corner.wait_recv()
    hand.append(send(block(1, 2), block(1, 2), to_tp(mate)))
    line_relay(1, 0)
    hand[1].wait_recv()
    up_rows(0, 1)
    hand[2].wait_recv()
    up_rows(1, 0)
    hand[3].wait_recv()
    up_rows(1, 1)

    peers = [(dy, dt) for dy in range(2) for dt in range(TP) if dy or dt]

    def chunk(k, j):
        def one(i, _):
            rs = pl.ds(pl.multiple_of(i * 2 * RT, 2 * RT), 2 * RT)
            part[k, rs, :] = dot(hidden[rs, :], down_buf[j]).astype(BF16)
            return 0

        lax.fori_loop(0, TP, one, 0)
        return [
            send(
                part.at[k, my_rows((y + dy) % 2 * TP + (tp + dt) % TP), :],
                part_in.at[k, dy * TP + dt - 1], group(dy, dt),
            )
            for dy, dt in peers
        ]

    def finish(k, j, copies):
        for copy in copies:
            copy.wait_recv()
        cs = pl.ds(pl.multiple_of(j * CB, CB), CB)
        acc = mid[:, cs].astype(F32) + part[k, my_rows(y * TP + tp), :].astype(F32)
        for d in range(2 * TP - 1):
            acc = acc + part_in[k, d].astype(F32)
        out[:, cs] = acc.astype(BF16)

    done = []
    for k in range(SP):
        d, dy = k // 2, (y + k) % 2
        if k == 4:
            line_relay(1, 1)
        j = line_arrived(1, dy, d) if d else at(0, dy)
        done.append((k, j, chunk(k, j)))
        if k > 1:
            finish(*done[k - 2])
    finish(*done[-2])
    finish(*done[-1])
    for when, copy in line_waits:
        @pl.when(when)
        def _(copy=copy):
            copy.wait_send()
    for copy in pending:
        copy.wait_send()


def one_kernel(SP, TP, *args):
    (stream, qw, kw, vw, gw, dw, qn, kn, vn, gn, dn, ow, on, gain, up, down) = args
    T = qw.shape[0]
    NB = T // BLOCK
    D = stream.shape[1]
    RT = T // TP
    FH = up.shape[1] // 2
    CB = down.shape[1]
    heads = dw.shape[0] + dn.shape[0]
    decay = jnp.concatenate([dw, dn]).reshape(heads * NB, BLOCK)
    decay = jnp.pad(decay, ((0, 128 - heads * NB), (0, 0)))
    offs, starts = turn_tables(SP, T)
    vmem = pl.BlockSpec(memory_space=pltpu.VMEM)
    hbm = pl.BlockSpec(memory_space=pl.ANY)
    copies = 96
    return pl.pallas_call(
        functools.partial(layer_kernel, SP, TP),
        out_shape=jax.ShapeDtypeStruct((RT, D), BF16),
        in_specs=[vmem] * 13 + [hbm] * 4,
        out_specs=vmem,
        scratch_shapes=[
            pltpu.VMEM((D, FH), BF16),
            pltpu.VMEM((SP, FH, CB), BF16),
            pltpu.VMEM((TP, 256, D), BF16),
            pltpu.VMEM((SP, 272, 128), BF16),
            pltpu.VMEM((T, 256), BF16),
            pltpu.VMEM((2, NB, 128, 128), F32),
            pltpu.VMEM((T, 256), F32),
            pltpu.VMEM((T, 256), BF16),
            pltpu.VMEM((TP, RT, 256), BF16),
            pltpu.VMEM((RT, D), BF16),
            pltpu.VMEM((2 * T, D), BF16),
            pltpu.VMEM((2 * T, FH), BF16),
            pltpu.VMEM((SP, 2 * T, CB), BF16),
            pltpu.VMEM((SP, 2 * TP - 1, RT, CB), BF16),
            pltpu.SemaphoreType.DMA((copies,)),
            pltpu.SemaphoreType.DMA((copies,)),
            pltpu.SemaphoreType.DMA((4,)),
            pltpu.SemaphoreType.DMA((20,)),
            pltpu.SemaphoreType.DMA((2 * SP,)),
        ],
        compiler_params=pltpu.CompilerParams(
            collective_id=0, has_side_effects=True, vmem_limit_bytes=60 * 1024 * 1024
        ),
    )(stream, qw, kw, vw, gw, qn, kn, vn, gn, decay, jnp.asarray(offs), jnp.asarray(starts),
      gain.reshape(1, D), ow, on, up, down)


def fits_kernel(SP, TP, args):
    D, FF = args[14].shape
    T = args[1].shape[0] // SP
    return (
        SP == 8 and TP == 4 and D % (SP * 128) == 0 and T % (TP * 32) == 0 and T % BLOCK == 0
        and args[1].shape[1] == TP * 128 and args[6].shape[1] == TP * 128
    )


def solution(mesh):
    in_specs = (
        P(("sp", "tp"), None),
        P("sp", "tp"),
        P("sp", "tp"),
        P("sp", "tp"),
        P("sp", "tp"),
        P("tp", "sp"),
        P("sp", "tp"),
        P("sp", "tp"),
        P("sp", "tp"),
        P("sp", "tp"),
        P("tp", "sp"),
        P("tp", None),
        P("tp", None),
        P(),
        P("sp", "tp"),
        P("tp", "sp"),
    )
    out_specs = P(("sp", "tp"), None)
    SP, TP = mesh.shape["sp"], mesh.shape["tp"]

    def layer(*args):
        body = functools.partial(one_kernel, SP, TP) if fits_kernel(SP, TP, args) else on_device
        return jax.shard_map(
            body, mesh=mesh, in_specs=in_specs, out_specs=out_specs, check_vma=False
        )(*args)

    return layer
```
